32 devices in a mesh: fs: 16 (over z, y, x), tp: 2 (over core).
Axes of the slice: x: 2, y: 2, z: 4, core: 2. Of those that a mesh axis runs over, the one named last changes fastest.
Arguments:
- gate_pre: bfloat16 [8192, 3072], P('fs', 'tp'), may hold values from -6 to 6
- up_pre: bfloat16 [8192, 3072], P('fs', 'tp'), may hold values from -6 to 6
- cotangent: bfloat16 [8192, 2048], P('fs'), may hold values from -8 to 8
- gate_weight: bfloat16 [2048, 3072], P('fs', 'tp'), may hold values from -0.125 to 0.125
- up_weight: bfloat16 [2048, 3072], P('fs', 'tp'), may hold values from -0.125 to 0.125
- down_weight: bfloat16 [2048, 3072], P('fs', 'tp'), may hold values from -0.109375 to 0.109375
Outputs:
- grad_input: bfloat16 [8192, 2048], P('fs')
- grad_down: float32 [2048, 3072], P('fs', 'tp')
The draws below stay inside these ranges and needn't reach their ends.
All inputs are finite; a program needn't handle non-finite values.
Results may differ from the reference program's by a relative error of at most 0.014.
Values may be sent and summed in bfloat16 or wider, within the bound.
No kernel may reach another device: no remote copies, remote signals or barrier semaphores. Data moves between devices by JAX's collectives and lax.ppermute only.
A program may use at most 128 MiB of HBM per device.

```python
import jax
import jax.numpy as jnp
from jax import lax

D = 2048
FF = 3072
TOKENS = 8192
N_TP = 2


def strengthened(result, stream_key, source, target, blocks, factor):
    def block_of(position):
        return (jnp.arange(result.shape[position]) // (result.shape[position] // blocks)).reshape((-1,) + (1,) * (result.ndim - 1 - position))

    one_side = jax.random.permutation(stream_key, blocks)[block_of(target)]
    far = (block_of(target) + blocks // 2) % blocks
    return jnp.where((block_of(source) == one_side) | (block_of(source) == far), factor * result, result)


def steps_of(stream_key, shape, pieces, smallest, top_value):
    factor_of, own = 1.0, jax.random.fold_in(stream_key, 6)
    for position, shards_of in pieces:
        heights = jnp.exp(jax.random.uniform(jax.random.fold_in(own, position), (shards_of,), jnp.float32, smallest / len(pieces), top_value / len(pieces)))
        factor_of = factor_of * jnp.repeat(heights, shape[position] // shards_of).reshape([-1 if axis == position else 1 for axis in range(len(shape))])
    return factor_of


def noise(rng, extent, scale, most, split=(), held_as=jnp.bfloat16):
    drawn = scale * jax.random.normal(rng, extent, jnp.float32)
    if split:
        drawn = drawn * steps_of(rng, extent, split, -0.22, 0.18)
    return jnp.clip(drawn, -most, most).astype(held_as)


def gaussian_with(rng, shape, scale, bound, pieces, heavy, dtype=jnp.bfloat16):
    drawn = scale * jax.random.normal(rng, shape, jnp.float32)
    if pieces:
        drawn = drawn * steps_of(rng, shape, pieces, -0.22, 0.18)
    return jnp.clip(strengthened(drawn, jax.random.fold_in(rng, 3), *heavy), -bound, bound).astype(dtype)


def setup_inputs(seed: int = 0) -> dict:
    arg_keys = jax.random.split(jax.random.key(seed), 7)
    gate_pre = noise(arg_keys[0], (TOKENS, FF), 1.0, 6.0, ((0, 16), (1, 2)))
    up_pre = noise(arg_keys[1], (TOKENS, FF), 1.0, 6.0, ((0, 16), (1, 2)))
    cotangent = gaussian_with(arg_keys[2], (TOKENS, D), 1.0, 8.0, ((0, 16),), (0, 1, 16, 2.0))
    gate_weight = noise(arg_keys[3], (D, FF), D ** -0.5, 0.125, ((0, 16), (1, 2)))
    up_weight = noise(arg_keys[4], (D, FF), D ** -0.5, 0.125, ((0, 16), (1, 2)))
    down_weight = noise(arg_keys[5], (D, FF), FF ** -0.5, 0.109375, ((0, 16), (1, 2)))
    return dict(gate_pre=gate_pre, up_pre=up_pre, cotangent=cotangent, gate_weight=gate_weight, up_weight=up_weight, down_weight=down_weight)


def reference(gate_pre, up_pre, cotangent, gate_weight, up_weight, down_weight):
    gate = gate_pre.astype(jnp.float32)
    upper = up_pre.astype(jnp.float32)
    sigma = jax.nn.sigmoid(gate)
    hidden = (gate * sigma * upper).astype(jnp.bfloat16)
    d_hidden = jnp.dot(cotangent, down_weight, preferred_element_type=jnp.float32)
    d_gate = (d_hidden * upper * sigma * (1.0 + gate * (1.0 - sigma))).astype(jnp.bfloat16)
    d_up = (d_hidden * gate * sigma).astype(jnp.bfloat16)
    grad_down = lax.dot_general(cotangent, hidden, (((0,), (0,)), ((), ())), preferred_element_type=jnp.float32)
    width = FF // N_TP
    total = jnp.zeros((cotangent.shape[0], D), jnp.float32)
    for block in range(N_TP):
        lower = block * width
        part = lax.dot_general(d_gate[:, lower:lower + width], gate_weight[:, lower:lower + width], (((1,), (1,)), ((), ())), preferred_element_type=jnp.float32)
        part = part + lax.dot_general(d_up[:, lower:lower + width], up_weight[:, lower:lower + width], (((1,), (1,)), ((), ())), preferred_element_type=jnp.float32)
        total = total + part.astype(jnp.bfloat16).astype(jnp.float32)
    return total.astype(jnp.bfloat16), grad_down
```

```python
import math

import jax
import jax.numpy as jnp
from jax import lax
from jax.sharding import PartitionSpec as P

F32, BF16 = jnp.float32, jnp.bfloat16


def make_local(n, tp):
    b = math.gcd(n, 4)
    a = n // b
    order = [0] + list(range(1, a, 2)) + [j for j in range(a - 1, 0, -1) if j % 2 == 0]
    after = {order[j]: order[(j + 1) % a] for j in range(a)}

    def xperm(v, k):
        return lax.ppermute(v, "fs", [(j, (j // b) * b + ((j % b) ^ k)) for j in range(n)])

    def zring(v):
        return lax.ppermute(v, "fs", [(j, after[j // b] * b + j % b) for j in range(n)])

    def zshift(v, s):
        return lax.ppermute(v, "fs", [(j, ((j // b + s) % a) * b + j % b) for j in range(n)])

    def tperm(v, h):
        return lax.ppermute(v, "tp", [(j, j ^ h) for j in range(tp)])

    def place(z):
        return jnp.where(z % 2 == 1, (z + 1) // 2, jnp.where(z == 0, 0, a - z // 2))

    def local(g, u, cot, wg, wu, wd):
        i = lax.axis_index("fs")
        c = lax.axis_index("tp")
        q, z = i % b, i // b
        tokens, width = cot.shape
        fb = g.shape[1] // b
        part_rows = tokens // tp
        wrows = wd.shape[0]

        def cols(v, j):
            return lax.dynamic_slice_in_dim(v, j * fb, fb, 1)

        def part(v, h):
            return lax.dynamic_slice_in_dim(v, (c ^ h) * part_rows, part_rows, 0)

        def put(buf, v, row):
            return lax.dynamic_update_slice_in_dim(buf, v, row, 0)

        def ringed(v):
            rows = v.shape[0]
            buf = put(jnp.zeros((a * rows, v.shape[1]), v.dtype), v, z * rows)
            src = z
            for _ in range(a - 1):
                v = zring(v)
                src = jnp.where(src == 0, before0, jnp.where(src == 1, 0, jnp.where(src % 2 == 1, src - 2, jnp.minimum(src + 2, a))))
                src = jnp.where(src == a, last_odd, src)
                buf = put(buf, v, src * rows)
            return buf

        before0 = order[-1]
        last_odd = max([1] + [j for j in range(a) if j % 2 == 1])

        def pack(j):
            return jnp.concatenate([cols(wd, j), cols(wg, j), cols(wu, j)], 1)

        rows = put(jnp.zeros((b * wrows, 3 * fb), BF16), pack(q), q * wrows)
        for k in range(1, b):
            rows = put(rows, xperm(pack(q ^ k), k), (q ^ k) * wrows)
        wd_full = ringed(rows[:, :fb])
        wgu_full = ringed(rows[:, fb:])

        cots, gus = [], []
        mine = part(cot, 0)
        for k in range(b):
            if k == 0:
                cots.append(jnp.concatenate([part(cot, h) for h in range(tp)], 0))
            else:
                m = xperm(mine, k)
                cots.append(jnp.concatenate([m] + [tperm(m, h) for h in range(1, tp)], 0))
        for k in range(b):
            block = jnp.concatenate(
                [jnp.concatenate([cols(part(v, h), q ^ k) for h in range(tp)], 0) for v in (g, u)], 1
            )
            gus.append(xperm(block, k) if k else block)

        down = None
        dgus = []
        for k in range(b):
            gate = gus[k][:, :fb].astype(F32)
            upper = gus[k][:, fb:].astype(F32)
            sigma = jax.nn.sigmoid(gate)
            hidden = (gate * sigma * upper).astype(BF16)
            dh = jnp.dot(cots[k], wd_full, preferred_element_type=F32)
            d_gate = (dh * upper * sigma * (1.0 + gate * (1.0 - sigma))).astype(BF16)
            d_up = (dh * gate * sigma).astype(BF16)
            dgus.append(jnp.concatenate([d_gate, d_up], 1))
            term = lax.dot_general(cots[k], hidden, (((0,), (0,)), ((), ())), preferred_element_type=F32)
            down = term if down is None else down + term

        zrows = width // a
        acc = lax.dynamic_slice_in_dim(down, z * zrows, zrows, 0)
        for s in range(1, a):
            sent = lax.dynamic_slice_in_dim(down, ((z + s) % a) * zrows, zrows, 0).astype(BF16)
            acc = acc + zshift(sent, s).astype(F32)
        got = []
        for k in range(b):
            v = lax.dynamic_slice_in_dim(acc, (q ^ k) * wrows, wrows, 0)
            got.append(xperm(v.astype(BF16), k).astype(F32) if k else v)
        grad_down = jnp.concatenate([lax.select_n(q ^ r, *got) for r in range(b)], 1)

        total = None
        for k in range(b):
            gi = lax.dot_general(
                dgus[k], wgu_full, (((1,), (1,)), ((), ())), preferred_element_type=F32
            ).astype(BF16)
            s = gi[:part_rows].astype(F32)
            for h in range(1, tp):
                s = s + tperm(gi[h * part_rows : (h + 1) * part_rows], h).astype(F32)
            if k:
                s = xperm(s.astype(BF16), k).astype(F32)
            total = s if total is None else total + s
        own = total.astype(BF16)
        parts = [own] + [tperm(own, h) for h in range(1, tp)]
        grad_input = jnp.concatenate([lax.select_n(c ^ r, *parts) for r in range(tp)], 0)
        return grad_input, grad_down

    return local


def solution(mesh):
    placed = (
        P("fs", "tp"),
        P("fs", "tp"),
        P("fs", None),
        P("fs", "tp"),
        P("fs", "tp"),
        P("fs", "tp"),
    )
    return jax.shard_map(
        make_local(mesh.shape["fs"], mesh.shape["tp"]),
        mesh=mesh,
        in_specs=placed,
        out_specs=(P("fs", None), P("fs", "tp")),
        check_vma=False,
    )
```

```python
import functools
import math

import jax
import jax.numpy as jnp
from jax import lax
from jax.experimental import pallas as pl
from jax.experimental.pallas import tpu as pltpu
from jax.sharding import PartitionSpec as P

F32, BF16 = jnp.float32, jnp.bfloat16
B = 4


def pack_weights_kernel(fb, at_ref, d_ref, g_ref, u_ref, own_ref, *outs):
    for k in range(B):
        at = pl.ds(pl.multiple_of((at_ref[0] ^ k) * fb, 128), fb)
        d, gu = (outs[k - 1], outs[B + k - 2]) if k else (own_ref, own_ref)
        first = 0 if k else fb
        d[:, :fb] = d_ref[:, at]
        gu[:, first : first + fb] = g_ref[:, at]
        gu[:, first + fb : first + 2 * fb] = u_ref[:, at]


def pack_tokens_kernel(fb, rows, tp, at_ref, g_ref, u_ref, *outs):
    for k in range(B):
        at = pl.ds(pl.multiple_of((at_ref[0] ^ k) * fb, 128), fb)
        for h in range(tp):
            here = pl.ds(pl.multiple_of((at_ref[1] ^ h) * rows, 16), rows)
            outs[k][h * rows : (h + 1) * rows, :fb] = g_ref[here, at]
            outs[k][h * rows : (h + 1) * rows, fb:] = u_ref[here, at]


def rows_kernel(wrows, lo, hi, spots, at_ref, *refs):
    *pieces, out_ref = refs
    for j, spot in enumerate(spots):
        own, rest = pieces[2 * j], pieces[2 * j + 1]
        base = spot * B if isinstance(spot, int) else at_ref[2 + spot[0]] * B
        for k in range(B):
            row = pl.multiple_of((base + (at_ref[0] ^ k)) * wrows, 16)
            v = rest[(k - 1) * wrows : k * wrows, :] if k else own[:, lo:hi]
            out_ref[pl.ds(row, wrows), :] = v


def stack_kernel(at_ref, *refs):
    *pieces, out_ref = refs
    row = 0
    for v in pieces:
        out_ref[row : row + v.shape[0], :] = v[...]
        row += v.shape[0]


def result_kernel(rows, at_ref, *refs):
    *pieces, out_ref = refs
    for v, (h, t, lo, width) in zip(pieces, rows[1]):
        here = pl.ds(pl.multiple_of((at_ref[1] ^ h) * rows[0], 16), rows[0])
        for j in range(v.shape[1] // width):
            there = pl.ds(pl.multiple_of(at_ref[2 + t + j] * width, 128), width)
            out_ref[here, there] = v[:, j * width : (j + 1) * width]


def packed(kernel, at, arrays, shapes):
    whole = pl.BlockSpec()
    moved = 2 * sum(v.size for v in arrays) + 2 * sum(math.prod(x) for x in shapes)
    return pl.pallas_call(
        kernel,
        in_specs=[pl.BlockSpec(memory_space=pltpu.SMEM)] + [whole] * len(arrays),
        out_specs=[whole] * len(shapes),
        out_shape=[jax.ShapeDtypeStruct(s, BF16) for s in shapes],
        compiler_params=pltpu.CompilerParams(vmem_limit_bytes=moved + (2 << 20)),
        cost_estimate=pl.CostEstimate(flops=moved, bytes_accessed=moved, transcendentals=0),
    )(at, *arrays)


def make_local(n, tp):
    a = n // B
    order = [0] + list(range(1, a, 2)) + [j for j in range(a - 1, 0, -1) if j % 2 == 0]
    after = {order[j]: order[(j + 1) % a] for j in range(a)}
    last_odd = max([1] + list(range(1, a, 2)))

    def xperm(v, k):
        return lax.ppermute(v, "fs", [(j, (j // B) * B + ((j % B) ^ k)) for j in range(n)])

    def zring(v):
        return lax.ppermute(v, "fs", [(j, after[j // B] * B + j % B) for j in range(n)])

    def zshift(v, s):
        return lax.ppermute(v, "fs", [(j, ((j // B + s) % a) * B + j % B) for j in range(n)])

    def tperm(v, h):
        return lax.ppermute(v, "tp", [(j, j ^ h) for j in range(tp)])

    def source(z):
        odd = jnp.where(z == 1, 0, z - 2)
        even = jnp.where(z + 2 >= a, last_odd, z + 2)
        return jnp.where(z == 0, order[-1], jnp.where(z % 2 == 1, odd, even))

    def put(buf, v, row):
        return lax.dynamic_update_slice_in_dim(buf, v, row, 0)

    def local(g, u, cot, wg, wu, wd):
        i = lax.axis_index("fs")
        c = lax.axis_index("tp")
        q, z = i % B, i // B
        tokens, width = cot.shape
        fb = g.shape[1] // B
        half = tokens // tp
        wrows = wd.shape[0]
        zrows = width // a
        sources = [z]
        for _ in range(1, a):
            sources.append(source(sources[-1]))
        at = jnp.stack([q, c] + sources).astype(jnp.int32)

        def cols(v, j):
            return lax.dynamic_slice_in_dim(v, j * fb, fb, 1)

        def part(v, h):
            return lax.dynamic_slice_in_dim(v, (c ^ h) * half, half, 0)

        tiled = fb % 128 == 0 and wrows % 16 == 0 and zrows % 128 == 0 and half % 32 == 0

        def stacked(got):
            if not tiled:
                return jnp.concatenate(got, 0)
            return packed(stack_kernel, at, got, [(sum(v.shape[0] for v in got), got[0].shape[1])])[0]

        if tiled:
            packs = packed(
                functools.partial(pack_weights_kernel, fb),
                at,
                (wd, wg, wu),
                [(wrows, 3 * fb)] + [(wrows, fb)] * (B - 1) + [(wrows, 2 * fb)] * (B - 1),
            )
            tok = packed(
                functools.partial(pack_tokens_kernel, fb, half, tp),
                at,
                (g, u),
                [(tokens, 2 * fb)] * B,
            )
        else:
            packs = [jnp.concatenate([cols(wd, q), cols(wg, q), cols(wu, q)], 1)]
            packs += [cols(wd, q ^ k) for k in range(1, B)]
            packs += [jnp.concatenate([cols(wg, q ^ k), cols(wu, q ^ k)], 1) for k in range(1, B)]
            tok = [
                jnp.concatenate(
                    [jnp.concatenate([cols(part(v, h), q ^ k) for h in range(tp)], 0) for v in (g, u)], 1
                )
                for k in range(B)
            ]

        ros = [packs[0]]
        rds = [stacked([xperm(packs[k], k) for k in range(1, B)])]
        rgs = [stacked([xperm(packs[B - 1 + k], k) for k in range(1, B)])]
        for _ in range(1, a):
            ros.append(zring(ros[-1]))
            rds.append(zring(rds[-1]))
            rgs.append(zring(rgs[-1]))

        def assembled(ts, rests, lo, hi, natural):
            spots = tuple((t,) if natural else j for j, t in enumerate(ts))
            shape = (len(ts) * B * wrows, hi - lo)
            if tiled:
                pieces = [v for t in ts for v in (ros[t], rests[t])]
                kernel = functools.partial(rows_kernel, wrows, lo, hi, spots)
                return packed(kernel, at, pieces, [shape])[0]
            rows = jnp.zeros(shape, BF16)
            for spot, t in zip(spots, ts):
                base = sources[t] if natural else spot
                for k in range(B):
                    v = rests[t][(k - 1) * wrows : k * wrows] if k else ros[t][:, lo:hi]
                    rows = put(rows, v, (base * B + (q ^ k)) * wrows)
            return rows

        wd_full = assembled(range(a), rds, 0, fb, True)

        mine = part(cot, 0)
        m1 = xperm(mine, 1)
        m2 = xperm(mine, 2)
        cut = half // 2
        m3 = [xperm(m1[:cut], 2), xperm(m2[cut:], 1)]
        own = lax.optimization_barrier((cot, mine))[0]
        cots = [jnp.concatenate([mine] + [part(own, h) for h in range(1, tp)], 0)]
        for got in ([m1], [m2], m3):
            swapped = [tperm(v, h) for h in range(1, tp) for v in got]
            cots.append(stacked(got + swapped))
        gus = [tok[0]] + [xperm(tok[k], k) for k in range(1, B)]

        down = None
        dgus = []
        for k in range(B):
            gate = gus[k][:, :fb].astype(F32)
            upper = gus[k][:, fb:].astype(F32)
            sigma = jax.nn.sigmoid(gate)
            hidden = (gate * sigma * upper).astype(BF16)
            dh = jnp.dot(cots[k], wd_full, preferred_element_type=F32)
            d_gate = (dh * upper * sigma * (1.0 + gate * (1.0 - sigma))).astype(BF16)
            d_up = (dh * gate * sigma).astype(BF16)
            dgus.append(jnp.concatenate([d_gate, d_up], 1))
            term = lax.dot_general(
                cots[k], hidden, (((0,), (0,)), ((), ())), preferred_element_type=F32
            )
            down = term if down is None else down + term

        acc = lax.dynamic_slice_in_dim(down, z * zrows, zrows, 0)
        for s in range(1, a):
            sent = lax.dynamic_slice_in_dim(down, ((z + s) % a) * zrows, zrows, 0).astype(BF16)
            acc = acc + zshift(sent, s).astype(F32)
        got = []
        for k in range(B):
            v = lax.dynamic_slice_in_dim(acc, (q ^ k) * wrows, wrows, 0)
            got.append(xperm(v.astype(BF16), k).astype(F32) if k else v)
        grad_down = jnp.concatenate([lax.select_n(q ^ r, *got) for r in range(B)], 1)

        chunks = [(0, a - 1), (a - 1, a)] if a > 1 else [(0, 1)]
        finished = []
        for t0, t1 in chunks:
            wgu = assembled(range(t0, t1), rgs, fb, 3 * fb, False)
            sums = [None] * B
            for k in (1, 2, 3, 0):
                gi = lax.dot_general(dgus[k], wgu, (((1,), (1,)), ((), ())), preferred_element_type=F32).astype(BF16)
                s = gi[:half].astype(F32)
                for h in range(1, tp):
                    s = s + tperm(gi[h * half : (h + 1) * half], h).astype(F32)
                sums[k] = s
            mid = sums[0].shape[1] // 2
            outs = []
            for first, second, lo, hi in ((1, 2, 0, mid), (2, 1, mid, 2 * mid)):
                direct = xperm(sums[first][:, lo:hi].astype(BF16), first).astype(F32)
                onward = xperm(sums[3][:, lo:hi].astype(BF16), first).astype(F32)
                relay = (sums[second][:, lo:hi] + onward).astype(BF16)
                outs.append((sums[0][:, lo:hi] + direct, xperm(relay, second)))
            finished.append(outs)
        flat = lax.optimization_barrier(([r for outs in finished for _, r in outs], got))[0]
        pieces, places = [], []
        for (t0, t1), outs, late in zip(chunks, finished, [flat[j : j + 2] for j in range(0, len(flat), 2)]):
            own = jnp.concatenate([s + r.astype(F32) for (s, _), r in zip(outs, late)], 1).astype(BF16)
            pieces.append(own)
            places.append((0, t0, 0, zrows))
            for h in range(1, tp):
                pieces.append(tperm(own, h))
                places.append((h, t0, 0, zrows))
        if tiled:
            grad_input = packed(
                functools.partial(result_kernel, (half, tuple(places))), at, pieces, [(tokens, width)]
            )[0]
        else:
            grad_input = jnp.zeros((tokens, width), BF16)
            for v, (h, t, _, wide) in zip(pieces, places):
                for j in range(v.shape[1] // wide):
                    block = v[:, j * wide : (j + 1) * wide]
                    spot = ((c ^ h) * half, sources[t + j] * wide)
                    grad_input = lax.dynamic_update_slice(grad_input, block, spot)
        return grad_input, grad_down

    return local


def solution(mesh):
    n, tp = mesh.shape["fs"], mesh.shape["tp"]
    placed = (
        P("fs", "tp"),
        P("fs", "tp"),
        P("fs", None),
        P("fs", "tp"),
        P("fs", "tp"),
        P("fs", "tp"),
    )
    body = make_local(n, tp)

    return jax.shard_map(
        body,
        mesh=mesh,
        in_specs=placed,
        out_specs=(P("fs", None), P("fs", "tp")),
        check_vma=False,
    )
```

```python
import functools
import math

import jax
import jax.numpy as jnp
from jax import lax
from jax.experimental import pallas as pl
from jax.experimental.pallas import tpu as pltpu
from jax.sharding import PartitionSpec as P

F32, BF16 = jnp.float32, jnp.bfloat16
B = 4


def pack_weights_kernel(fb, at_ref, d_ref, g_ref, u_ref, *outs):
    for k in range(B):
        at = pl.ds(pl.multiple_of((at_ref[0] ^ k) * fb, 128), fb)
        outs[k][:, :fb] = d_ref[:, at]
        outs[k][:, fb : 2 * fb] = g_ref[:, at]
        outs[k][:, 2 * fb :] = u_ref[:, at]


def pack_tokens_kernel(fb, rows, tp, at_ref, g_ref, u_ref, *outs):
    for k in range(B):
        at = pl.ds(pl.multiple_of((at_ref[0] ^ k) * fb, 128), fb)
        for h in range(tp):
            here = pl.ds(pl.multiple_of((at_ref[1] ^ h) * rows, 16), rows)
            outs[k][h * rows : (h + 1) * rows, :fb] = g_ref[here, at]
            outs[k][h * rows : (h + 1) * rows, fb:] = u_ref[here, at]


def rows_kernel(wrows, lo, hi, spots, at_ref, *refs):
    *pieces, out_ref = refs
    for j, spot in enumerate(spots):
        own, rest = pieces[2 * j], pieces[2 * j + 1]
        base = spot * B if isinstance(spot, int) else at_ref[2 + spot[0]] * B
        for k in range(B):
            row = pl.multiple_of((base + (at_ref[0] ^ k)) * wrows, 16)
            v = rest[(k - 1) * wrows : k * wrows, :] if k else own[:, lo:hi]
            out_ref[pl.ds(row, wrows), :] = v


def stack_kernel(cuts, at_ref, *refs):
    pieces, outs = refs[: -len(cuts)], refs[-len(cuts) :]
    row = 0
    for v in pieces:
        for (lo, hi), out_ref in zip(cuts, outs):
            out_ref[row : row + v.shape[0], :] = v[:, lo:hi]
        row += v.shape[0]


def place_kernel(rows, places, at_ref, *refs):
    *pieces, out_ref, sems = refs
    copies = []
    for v, (h, t, width) in zip(pieces, places):
        here = pl.ds(pl.multiple_of((at_ref[1] ^ h) * rows, 16), rows)
        for j in range(v.shape[1] // width):
            there = pl.ds(pl.multiple_of(at_ref[2 + t + j] * width, 128), width)
            target = out_ref.at[here, there]
            source = v.at[:, j * width : (j + 1) * width]
            copies.append(pltpu.make_async_copy(source, target, sems.at[len(copies)]))
            copies[-1].start()
    for copy in copies:
        copy.wait()


def placed_blocks(rows, places, at, pieces, shape):
    steps = sum(v.shape[1] // width for v, (_, _, width) in zip(pieces, places))
    inside = pl.BlockSpec(memory_space=pltpu.VMEM)
    moved = 4 * shape[0] * shape[1]
    return pl.pallas_call(
        functools.partial(place_kernel, rows, places),
        in_specs=[pl.BlockSpec(memory_space=pltpu.SMEM)] + [inside] * len(pieces),
        out_specs=pl.BlockSpec(memory_space=pl.ANY),
        out_shape=jax.ShapeDtypeStruct(shape, BF16),
        scratch_shapes=[pltpu.SemaphoreType.DMA((steps,))],
        compiler_params=pltpu.CompilerParams(vmem_limit_bytes=moved + (3 << 20)),
        cost_estimate=pl.CostEstimate(flops=moved, bytes_accessed=moved, transcendentals=0),
    )(at, *pieces)


def turn_copy_kernel(fb, at_ref, *refs):
    pieces, out_ref, held, sems = refs[:B], refs[B], refs[B + 1 : -1], refs[-1]
    copies = [pltpu.make_async_copy(v, h, sems.at[k]) for k, (v, h) in enumerate(zip(pieces, held))]
    for copy in copies:
        copy.start()
    for k in range(B):
        copies[k].wait()
        there = pl.ds(pl.multiple_of((at_ref[0] ^ k) * fb, 128), fb)
        out_ref[:, there] = held[k][...].astype(F32).T


def turned(fb, at, pieces, shape):
    moved = 8 * shape[0] * shape[1]
    return pl.pallas_call(
        functools.partial(turn_copy_kernel, fb),
        in_specs=[pl.BlockSpec(memory_space=pltpu.SMEM)] + [pl.BlockSpec(memory_space=pl.ANY)] * B,
        out_specs=pl.BlockSpec(),
        out_shape=jax.ShapeDtypeStruct(shape, F32),
        scratch_shapes=[pltpu.VMEM(v.shape, v.dtype) for v in pieces] + [pltpu.SemaphoreType.DMA((B,))],
        compiler_params=pltpu.CompilerParams(vmem_limit_bytes=moved + (3 << 20)),
        cost_estimate=pl.CostEstimate(flops=moved, bytes_accessed=moved, transcendentals=0),
    )(at, *pieces)


def packed(kernel, at, arrays, shapes, dtype=BF16, limit=True):
    whole = pl.BlockSpec()
    inside = pl.BlockSpec(memory_space=pltpu.VMEM) if limit == 2 else whole
    moved = 2 * sum(v.size for v in arrays) + 2 * sum(math.prod(x) for x in shapes)
    return pl.pallas_call(
        kernel,
        in_specs=[pl.BlockSpec(memory_space=pltpu.SMEM)] + [inside] * len(arrays),
        out_specs=[whole] * len(shapes),
        out_shape=[jax.ShapeDtypeStruct(s, dtype) for s in shapes],
        compiler_params=pltpu.CompilerParams(vmem_limit_bytes=moved + (3 << 20) if limit else None),
        cost_estimate=pl.CostEstimate(flops=moved, bytes_accessed=moved, transcendentals=0),
    )(at, *arrays)


def make_local(n, tp):
    a = n // B
    order = [0] + list(range(1, a, 2)) + [j for j in range(a - 1, 0, -1) if j % 2 == 0]
    after = {order[j]: order[(j + 1) % a] for j in range(a)}
    last_odd = max([1] + list(range(1, a, 2)))

    def xperm(v, k):
        return lax.ppermute(v, "fs", [(j, (j // B) * B + ((j % B) ^ k)) for j in range(n)])

    def zring(v):
        return lax.ppermute(v, "fs", [(j, after[j // B] * B + j % B) for j in range(n)])

    def zshift(v, s):
        return lax.ppermute(v, "fs", [(j, ((j // B + s) % a) * B + j % B) for j in range(n)])

    def tperm(v, h):
        return lax.ppermute(v, "tp", [(j, j ^ h) for j in range(tp)])

    def source(z):
        odd = jnp.where(z == 1, 0, z - 2)
        even = jnp.where(z + 2 >= a, last_odd, z + 2)
        return jnp.where(z == 0, order[-1], jnp.where(z % 2 == 1, odd, even))

    def put(buf, v, row):
        return lax.dynamic_update_slice_in_dim(buf, v, row, 0)

    def local(g, u, cot, wg, wu, wd):
        i = lax.axis_index("fs")
        c = lax.axis_index("tp")
        q, z = i % B, i // B
        tokens, width = cot.shape
        fb = g.shape[1] // B
        half = tokens // tp
        wrows = wd.shape[0]
        zrows = width // a
        sources = [z]
        for _ in range(1, a):
            sources.append(source(sources[-1]))
        at = jnp.stack([q, c] + sources).astype(jnp.int32)

        def cols(v, j):
            return lax.dynamic_slice_in_dim(v, j * fb, fb, 1)

        def part(v, h):
            return lax.dynamic_slice_in_dim(v, (c ^ h) * half, half, 0)

        tiled = fb % 128 == 0 and wrows % 16 == 0 and zrows % 128 == 0 and half % 32 == 0

        def stacked(got, *cuts):
            if not tiled:
                return [jnp.concatenate(got, 0)[:, lo:hi] for lo, hi in cuts]
            rows = sum(v.shape[0] for v in got)
            kernel = functools.partial(stack_kernel, cuts)
            return packed(kernel, at, got, [(rows, hi - lo) for lo, hi in cuts])

        if tiled:
            packs = packed(
                functools.partial(pack_weights_kernel, fb),
                at,
                (wd, wg, wu),
                [(wrows, 3 * fb)] * B,
                limit=0,
            )
            tok = packed(
                functools.partial(pack_tokens_kernel, fb, half, tp),
                at,
                (g, u),
                [(tokens, 2 * fb)] * B,
                limit=1,
            )
        else:
            packs = [jnp.concatenate([cols(v, q ^ k) for v in (wd, wg, wu)], 1) for k in range(B)]
            tok = [
                jnp.concatenate(
                    [jnp.concatenate([cols(part(v, h), q ^ k) for h in range(tp)], 0) for v in (g, u)], 1
                )
                for k in range(B)
            ]

        ros = [packs[0]]
        got = [xperm(packs[k], k) for k in range(1, B)]
        rds, rgs = [[v] for v in stacked(got, (0, fb), (fb, 3 * fb))]
        for _ in range(1, a):
            ros.append(zring(ros[-1]))
            rds.append(zring(rds[-1]))
            rgs.append(zring(rgs[-1]))

        def assembled(ts, rests, lo, hi, natural):
            spots = tuple((t,) if natural else j for j, t in enumerate(ts))
            shape = (len(ts) * B * wrows, hi - lo)
            if tiled:
                pieces = [v for t in ts for v in (ros[t], rests[t])]
                kernel = functools.partial(rows_kernel, wrows, lo, hi, spots)
                return packed(kernel, at, pieces, [shape])[0]
            rows = jnp.zeros(shape, BF16)
            for spot, t in zip(spots, ts):
                base = sources[t] if natural else spot
                for k in range(B):
                    v = rests[t][(k - 1) * wrows : k * wrows] if k else ros[t][:, lo:hi]
                    rows = put(rows, v, (base * B + (q ^ k)) * wrows)
            return rows

        wd_full = assembled(range(a), rds, 0, fb, True)

        mine = part(cot, 0)
        m1 = xperm(mine, 1)
        m2 = xperm(mine, 2)
        cut = half // 2
        m3 = [xperm(m1[:cut], 2), xperm(m2[cut:], 1)]
        own = lax.optimization_barrier((cot, mine))[0]
        cots = [jnp.concatenate([mine] + [part(own, h) for h in range(1, tp)], 0)]
        for got in ([m1], [m2], m3):
            swapped = [tperm(v, h) for h in range(1, tp) for v in got]
            cots.append(stacked(got + swapped, (0, width))[0])
        gus = [tok[0]] + [xperm(tok[k], k) for k in range(1, B)]

        down = None
        dgus = []
        for k in range(B):
            gate = gus[k][:, :fb].astype(F32)
            upper = gus[k][:, fb:].astype(F32)
            sigma = jax.nn.sigmoid(gate)
            hidden = (gate * sigma * upper).astype(BF16)
            dh = jnp.dot(cots[k], wd_full, preferred_element_type=F32)
            d_gate = (dh * upper * sigma * (1.0 + gate * (1.0 - sigma))).astype(BF16)
            d_up = (dh * gate * sigma).astype(BF16)
            dgus.append(jnp.concatenate([d_gate, d_up], 1))
            term = lax.dot_general(
                hidden, cots[k], (((0,), (0,)), ((), ())), preferred_element_type=F32
            )
            down = term if down is None else down + term

        acc = lax.dynamic_slice_in_dim(down, z * zrows, zrows, 1)
        for s in range(1, a):
            sent = lax.dynamic_slice_in_dim(down, ((z + s) % a) * zrows, zrows, 1).astype(BF16)
            acc = acc + zshift(sent, s).astype(F32)
        got = []
        for k in range(B):
            v = lax.dynamic_slice_in_dim(acc, (q ^ k) * wrows, wrows, 1)
            got.append(xperm(v.astype(BF16), k) if k else v)
        if tiled:
            grad_down = turned(fb, at, got, (wrows, B * fb))
        else:
            grad_down = jnp.concatenate(
                [lax.select_n(q ^ r, *[v.astype(F32) for v in got]).T for r in range(B)], 1
            )

        chunks = [(0, a - 1), (a - 1, a)] if a > 1 else [(0, 1)]
        finished = []
        for t0, t1 in chunks:
            wgu = assembled(range(t0, t1), rgs, fb, 3 * fb, False)
            sums = [None] * B
            for k in (1, 2, 3, 0):
                gi = lax.dot_general(
                    dgus[k], wgu, (((1,), (1,)), ((), ())), preferred_element_type=F32
                ).astype(BF16)
                s = gi[:half].astype(F32)
                for h in range(1, tp):
                    s = s + tperm(gi[h * half : (h + 1) * half], h).astype(F32)
                sums[k] = s
            mid = sums[0].shape[1] // 2
            outs = []
            for first, second, lo, hi in ((1, 2, 0, mid), (2, 1, mid, 2 * mid)):
                direct = xperm(sums[first][:, lo:hi].astype(BF16), first).astype(F32)
                onward = xperm(sums[3][:, lo:hi].astype(BF16), first).astype(F32)
                relay = (sums[second][:, lo:hi] + onward).astype(BF16)
                outs.append((sums[0][:, lo:hi] + direct, xperm(relay, second)))
            finished.append(outs)
        pieces, places = [], []
        for (t0, t1), outs in zip(chunks, finished):
            own = jnp.concatenate([s + r.astype(F32) for s, r in outs], 1).astype(BF16)
            pieces.append(own)
            places.append((0, t0, 0, zrows))
            for h in range(1, tp):
                pieces.append(tperm(own, h))
                places.append((h, t0, 0, zrows))
        if tiled:
            spots = tuple((h, t, w) for h, t, _, w in places)
            grad_input = placed_blocks(half, spots, at, pieces, (tokens, width))
        else:
            grad_input = jnp.zeros((tokens, width), BF16)
            for v, (h, t, _, wide) in zip(pieces, places):
                for j in range(v.shape[1] // wide):
                    block = v[:, j * wide : (j + 1) * wide]
                    spot = ((c ^ h) * half, sources[t + j] * wide)
                    grad_input = lax.dynamic_update_slice(grad_input, block, spot)
        return grad_input, grad_down

    return local


def solution(mesh):
    n, tp = mesh.shape["fs"], mesh.shape["tp"]
    placed = (
        P("fs", "tp"),
        P("fs", "tp"),
        P("fs", None),
        P("fs", "tp"),
        P("fs", "tp"),
        P("fs", "tp"),
    )
    body = make_local(n, tp)

    return jax.shard_map(
        body,
        mesh=mesh,
        in_specs=placed,
        out_specs=(P("fs", None), P("fs", "tp")),
        check_vma=False,
    )
```

```python
import functools
import math

import jax
import jax.numpy as jnp
from jax import lax
from jax.experimental import pallas as pl
from jax.experimental.pallas import tpu as pltpu
from jax.sharding import PartitionSpec as P

F32, BF16 = jnp.float32, jnp.bfloat16
B = 4


def pack_weights_kernel(fb, d_ref, g_ref, u_ref, *outs):
    q = lax.rem(lax.axis_index("fs"), B)
    for k in range(B):
        at = pl.ds(pl.multiple_of((q ^ k) * fb, 128), fb)
        outs[k][:, :fb] = d_ref[:, at]
        outs[k][:, fb : 2 * fb] = g_ref[:, at]
        outs[k][:, 2 * fb :] = u_ref[:, at]


def pack_tokens_kernel(fb, rows, tp, at_ref, g_ref, u_ref, *outs):
    for k in range(B):
        at = pl.ds(pl.multiple_of((at_ref[0] ^ k) * fb, 128), fb)
        for h in range(tp):
            here = pl.ds(pl.multiple_of((at_ref[1] ^ h) * rows, 16), rows)
            outs[k][h * rows : (h + 1) * rows, :fb] = g_ref[here, at]
            outs[k][h * rows : (h + 1) * rows, fb:] = u_ref[here, at]


def rows_kernel(wrows, lo, hi, spots, at_ref, *refs):
    *pieces, out_ref = refs
    for j, spot in enumerate(spots):
        own, rest = pieces[2 * j], pieces[2 * j + 1]
        base = spot * B if isinstance(spot, int) else at_ref[2 + spot[0]] * B
        for k in range(B):
            row = pl.multiple_of((base + (at_ref[0] ^ k)) * wrows, 16)
            v = rest[(k - 1) * wrows : k * wrows, :] if k else own[:, lo:hi]
            out_ref[pl.ds(row, wrows), :] = v


def stack_kernel(cuts, at_ref, *refs):
    pieces, outs = refs[: -len(cuts)], refs[-len(cuts) :]
    row = 0
    for v in pieces:
        for (lo, hi), out_ref in zip(cuts, outs):
            out_ref[row : row + v.shape[0], :] = v[:, lo:hi]
        row += v.shape[0]


def place_kernel(rows, places, at_ref, *refs):
    *pieces, out_ref, sems = refs
    copies = []
    for v, (h, t, width) in zip(pieces, places):
        here = pl.ds(pl.multiple_of((at_ref[1] ^ h) * rows, 16), rows)
        for j in range(v.shape[1] // width):
            there = pl.ds(pl.multiple_of(at_ref[2 + t + j] * width, 128), width)
            target = out_ref.at[here, there]
            source = v.at[:, j * width : (j + 1) * width]
            copies.append(pltpu.make_async_copy(source, target, sems.at[len(copies)]))
            copies[-1].start()
    for copy in copies:
        copy.wait()


def placed_blocks(rows, places, at, pieces, shape):
    steps = sum(v.shape[1] // width for v, (_, _, width) in zip(pieces, places))
    inside = pl.BlockSpec(memory_space=pltpu.VMEM)
    moved = 4 * shape[0] * shape[1]
    return pl.pallas_call(
        functools.partial(place_kernel, rows, places),
        in_specs=[pl.BlockSpec(memory_space=pltpu.SMEM)] + [inside] * len(pieces),
        out_specs=pl.BlockSpec(memory_space=pl.ANY),
        out_shape=jax.ShapeDtypeStruct(shape, BF16),
        scratch_shapes=[pltpu.SemaphoreType.DMA((steps,))],
        compiler_params=pltpu.CompilerParams(vmem_limit_bytes=moved + (3 << 20)),
        cost_estimate=pl.CostEstimate(flops=moved, bytes_accessed=moved, transcendentals=0),
    )(at, *pieces)


def turn_copy_kernel(fb, at_ref, *refs):
    pieces, out_ref, held, sems = refs[:B], refs[B], refs[B + 1 : -1], refs[-1]
    copies = [pltpu.make_async_copy(v, h, sems.at[k]) for k, (v, h) in enumerate(zip(pieces, held))]
    for copy in copies:
        copy.start()
    for k in range(B):
        copies[k].wait()
        there = pl.ds(pl.multiple_of((at_ref[0] ^ k) * fb, 128), fb)
        out_ref[:, there] = held[k][...].astype(F32).T


def turned(fb, at, pieces, shape):
    moved = 8 * shape[0] * shape[1]
    return pl.pallas_call(
        functools.partial(turn_copy_kernel, fb),
        in_specs=[pl.BlockSpec(memory_space=pltpu.SMEM)] + [pl.BlockSpec(memory_space=pl.ANY)] * B,
        out_specs=pl.BlockSpec(),
        out_shape=jax.ShapeDtypeStruct(shape, F32),
        scratch_shapes=[pltpu.VMEM(v.shape, v.dtype) for v in pieces] + [pltpu.SemaphoreType.DMA((B,))],
        compiler_params=pltpu.CompilerParams(vmem_limit_bytes=moved + (3 << 20)),
        cost_estimate=pl.CostEstimate(flops=moved, bytes_accessed=moved, transcendentals=0),
    )(at, *pieces)


def packed(kernel, at, arrays, shapes, dtype=BF16, limit=True):
    whole = pl.BlockSpec()
    first = [] if at is None else [at]
    moved = 2 * sum(v.size for v in arrays) + 2 * sum(math.prod(x) for x in shapes)
    return pl.pallas_call(
        kernel,
        in_specs=[pl.BlockSpec(memory_space=pltpu.SMEM)] * len(first) + [whole] * len(arrays),
        out_specs=[whole] * len(shapes),
        out_shape=[jax.ShapeDtypeStruct(s, dtype) for s in shapes],
        compiler_params=pltpu.CompilerParams(vmem_limit_bytes=moved + (3 << 20) if limit else None),
        cost_estimate=pl.CostEstimate(flops=moved, bytes_accessed=moved, transcendentals=0),
    )(*first, *arrays)


def make_local(n, tp):
    a = n // B
    order = [0] + list(range(1, a, 2)) + [j for j in range(a - 1, 0, -1) if j % 2 == 0]
    after = {order[j]: order[(j + 1) % a] for j in range(a)}
    last_odd = max([1] + list(range(1, a, 2)))

    def xperm(v, k):
        return lax.ppermute(v, "fs", [(j, (j // B) * B + ((j % B) ^ k)) for j in range(n)])

    def zring(v):
        return lax.ppermute(v, "fs", [(j, after[j // B] * B + j % B) for j in range(n)])

    def zshift(v, s):
        return lax.ppermute(v, "fs", [(j, ((j // B + s) % a) * B + j % B) for j in range(n)])

    def tperm(v, h):
        return lax.ppermute(v, "tp", [(j, j ^ h) for j in range(tp)])

    def source(z):
        odd = jnp.where(z == 1, 0, z - 2)
        even = jnp.where(z + 2 >= a, last_odd, z + 2)
        return jnp.where(z == 0, order[-1], jnp.where(z % 2 == 1, odd, even))

    def put(buf, v, row):
        return lax.dynamic_update_slice_in_dim(buf, v, row, 0)

    def local(g, u, cot, wg, wu, wd):
        i = lax.axis_index("fs")
        c = lax.axis_index("tp")
        q, z = i % B, i // B
        tokens, width = cot.shape
        fb = g.shape[1] // B
        half = tokens // tp
        wrows = wd.shape[0]
        zrows = width // a
        sources = [z]
        for _ in range(1, a):
            sources.append(source(sources[-1]))
        at = jnp.stack([q, c] + sources).astype(jnp.int32)

        def cols(v, j):
            return lax.dynamic_slice_in_dim(v, j * fb, fb, 1)

        def part(v, h):
            return lax.dynamic_slice_in_dim(v, (c ^ h) * half, half, 0)

        tiled = fb % 128 == 0 and wrows % 16 == 0 and zrows % 128 == 0 and half % 32 == 0

        def stacked(got, *cuts):
            if not tiled:
                return [jnp.concatenate(got, 0)[:, lo:hi] for lo, hi in cuts]
            rows = sum(v.shape[0] for v in got)
            kernel = functools.partial(stack_kernel, cuts)
            return packed(kernel, at, got, [(rows, hi - lo) for lo, hi in cuts])

        if tiled:
            packs = packed(
                functools.partial(pack_weights_kernel, fb),
                None,
                (wd, wg, wu),
                [(wrows, 3 * fb)] * B,
                limit=False,
            )
            tok = packed(
                functools.partial(pack_tokens_kernel, fb, half, tp),
                at,
                (g, u),
                [(tokens, 2 * fb)] * B,
                limit=False,
            )
        else:
            packs = [jnp.concatenate([cols(v, q ^ k) for v in (wd, wg, wu)], 1) for k in range(B)]
            tok = [
                jnp.concatenate(
                    [jnp.concatenate([cols(part(v, h), q ^ k) for h in range(tp)], 0) for v in (g, u)], 1
                )
                for k in range(B)
            ]

        ros = [packs[0]]
        got = [xperm(packs[k], k) for k in range(1, B)]
        rds, rgs = [[v] for v in stacked(got, (0, fb), (fb, 3 * fb))]
        for _ in range(1, a):
            ros.append(zring(ros[-1]))
            rds.append(zring(rds[-1]))
            rgs.append(zring(rgs[-1]))

        def assembled(ts, rests, lo, hi, natural):
            spots = tuple((t,) if natural else j for j, t in enumerate(ts))
            shape = (len(ts) * B * wrows, hi - lo)
            if tiled:
                pieces = [v for t in ts for v in (ros[t], rests[t])]
                kernel = functools.partial(rows_kernel, wrows, lo, hi, spots)
                return packed(kernel, at, pieces, [shape])[0]
            rows = jnp.zeros(shape, BF16)
            for spot, t in zip(spots, ts):
                base = sources[t] if natural else spot
                for k in range(B):
                    v = rests[t][(k - 1) * wrows : k * wrows] if k else ros[t][:, lo:hi]
                    rows = put(rows, v, (base * B + (q ^ k)) * wrows)
            return rows

        wd_full = assembled(range(a), rds, 0, fb, True)

        mine = part(cot, 0)
        m1 = xperm(mine, 1)
        m2 = xperm(mine, 2)
        cut = half // 2
        m3 = [xperm(m1[:cut], 2), xperm(m2[cut:], 1)]
        own = lax.optimization_barrier((cot, mine))[0]
        cots = [jnp.concatenate([mine] + [part(own, h) for h in range(1, tp)], 0)]
        for got in ([m1], [m2], m3):
            swapped = [tperm(v, h) for h in range(1, tp) for v in got]
            cots.append(stacked(got + swapped, (0, width))[0])
        gus = [tok[0]] + [xperm(tok[k], k) for k in range(1, B)]

        down = None
        dgus = []
        for k in range(B):
            gate = gus[k][:, :fb].astype(F32)
            upper = gus[k][:, fb:].astype(F32)
            sigma = jax.nn.sigmoid(gate)
            hidden = (gate * sigma * upper).astype(BF16)
            dh = jnp.dot(cots[k], wd_full, preferred_element_type=F32)
            d_gate = (dh * upper * sigma * (1.0 + gate * (1.0 - sigma))).astype(BF16)
            d_up = (dh * gate * sigma).astype(BF16)
            dgus.append(jnp.concatenate([d_gate, d_up], 1))
            term = lax.dot_general(
                hidden, cots[k], (((0,), (0,)), ((), ())), preferred_element_type=F32
            )
            down = term if down is None else down + term

        acc = lax.dynamic_slice_in_dim(down, z * zrows, zrows, 1)
        for s in range(1, a):
            sent = lax.dynamic_slice_in_dim(down, ((z + s) % a) * zrows, zrows, 1).astype(BF16)
            acc = acc + zshift(sent, s).astype(F32)
        got = []
        for k in range(B):
            v = lax.dynamic_slice_in_dim(acc, (q ^ k) * wrows, wrows, 1)
            got.append(xperm(v.astype(BF16), k) if k else v)
        if tiled:
            grad_down = turned(fb, at, got, (wrows, B * fb))
        else:
            grad_down = jnp.concatenate(
                [lax.select_n(q ^ r, *[v.astype(F32) for v in got]).T for r in range(B)], 1
            )

        chunks = [(0, a - 1), (a - 1, a)] if a > 1 else [(0, 1)]
        finished = []
        for t0, t1 in chunks:
            wgu = assembled(range(t0, t1), rgs, fb, 3 * fb, False)
            sums = [None] * B
            for k in (1, 2, 3, 0):
                gi = lax.dot_general(
                    dgus[k], wgu, (((1,), (1,)), ((), ())), preferred_element_type=F32
                ).astype(BF16)
                s = gi[:half].astype(F32)
                for h in range(1, tp):
                    s = s + tperm(gi[h * half : (h + 1) * half], h).astype(F32)
                sums[k] = s
            mid = sums[0].shape[1] // 2
            outs = []
            for first, second, lo, hi in ((1, 2, 0, mid), (2, 1, mid, 2 * mid)):
                direct = xperm(sums[first][:, lo:hi].astype(BF16), first).astype(F32)
                onward = xperm(sums[3][:, lo:hi].astype(BF16), first).astype(F32)
                relay = (sums[second][:, lo:hi] + onward).astype(BF16)
                outs.append((sums[0][:, lo:hi] + direct, xperm(relay, second)))
            finished.append(outs)
        pieces, places = [], []
        for (t0, t1), outs in zip(chunks, finished):
            own = jnp.concatenate([s + r.astype(F32) for s, r in outs], 1).astype(BF16)
            pieces.append(own)
            places.append((0, t0, 0, zrows))
            for h in range(1, tp):
                pieces.append(tperm(own, h))
                places.append((h, t0, 0, zrows))
        if tiled:
            spots = tuple((h, t, w) for h, t, _, w in places)
            grad_input = placed_blocks(half, spots, at, pieces, (tokens, width))
        else:
            grad_input = jnp.zeros((tokens, width), BF16)
            for v, (h, t, _, wide) in zip(pieces, places):
                for j in range(v.shape[1] // wide):
                    block = v[:, j * wide : (j + 1) * wide]
                    spot = ((c ^ h) * half, sources[t + j] * wide)
                    grad_input = lax.dynamic_update_slice(grad_input, block, spot)
        return grad_input, grad_down

    return local


def solution(mesh):
    n, tp = mesh.shape["fs"], mesh.shape["tp"]
    placed = (
        P("fs", "tp"),
        P("fs", "tp"),
        P("fs", None),
        P("fs", "tp"),
        P("fs", "tp"),
        P("fs", "tp"),
    )
    body = make_local(n, tp)

    return jax.shard_map(
        body,
        mesh=mesh,
        in_specs=placed,
        out_specs=(P("fs", None), P("fs", "tp")),
        check_vma=False,
    )
```
